32 devices in a mesh: ep: 32 (over z, y, x, core).
Axes of the slice: x: 2, y: 2, z: 4, core: 2. Of those that a mesh axis runs over, the one named last changes fastest.
Arguments:
- latest_embeddings: bfloat16 [512, 2048], P('ep'), may hold values from -6 to 6
- prior_memory_grids: float32 [512, 32, 4096], P('ep'), may hold values from -1.75 to 1.75
- earlier_rescale_gain: float32 [2048], replicated, may hold values from 0.1 to 1.9
- query_map: bfloat16 [2048, 2048], P(None, 'ep'), may hold values from -0.125 to 0.125
- lookup_map: bfloat16 [2048, 2048], P(None, 'ep'), may hold values from -0.125 to 0.125
- content_map: bfloat16 [2048, 2048], P(None, 'ep'), may hold values from -0.125 to 0.125
- forget_lower_map: bfloat16 [2048, 64], replicated, may hold values from -0.125 to 0.125
- forget_upper_map: bfloat16 [64, 2048], replicated, may hold values from -0.75 to 0.75
- forget_shift: float32 [2048], replicated, may hold values from -3 to 3
- adapt_lower_map: bfloat16 [2048, 64], replicated, may hold values from -0.125 to 0.125
- adapt_upper_map: bfloat16 [64, 2048], replicated, may hold values from -0.75 to 0.75
- adapt_shift: float32 [2048], replicated, may hold values from -2 to 2
- erase_lookup_gains: float32 [2048], replicated, may hold values from 0.1 to 1.9
- substitute_lookup_gains: float32 [2048], replicated, may hold values from 0.1 to 1.9
- present_extra_gains: float32 [2048], replicated, may hold values from -1.75 to 1.75
- attender_rescale_gain: float32 [2048], replicated, may hold values from 0.1 to 1.9
- result_map: bfloat16 [2048, 2048], P(None, 'ep'), may hold values from -0.125 to 0.125
- later_rescale_gain: float32 [2048], replicated, may hold values from 0.1 to 1.9
- specialist_switch_maps: bfloat16 [32, 2048, 512], P('ep'), may hold values from -0.125 to 0.125
- specialist_widen_maps: bfloat16 [32, 2048, 512], P('ep'), may hold values from -0.125 to 0.125
- specialist_shrink_maps: bfloat16 [32, 512, 2048], P('ep'), may hold values from -0.25 to 0.25
- picked_specialists: int32 [512, 6], P('ep'), may hold values from 0 to 31, as said below
- specialist_picked_shares: float32 [512, 6], P('ep'), may hold values from 0.02 to 0.5
Outputs:
- new_hidden: bfloat16 [512, 2048], P('ep')
- new_state: float32 [512, 32, 4096], P('ep')
The draws below stay inside these ranges and needn't reach their ends.
Inputs may be any that keep to these rules, and one draw needn't show every extreme that they name: `picked_specialists`: each row names 6 different experts of one group; a group is a run of 8 consecutive expert numbers. The rows of one device use exactly two groups, one of them for half of the device's rows rounded up and the other for the rest. No expert is named by more than 6 rows of one device, and on every device some expert is named by exactly 6.
All inputs are finite; a program needn't handle non-finite values.
Results may differ from the reference program's by a relative error of at most 0.011.
Values may be sent and summed in bfloat16 or wider, within the bound.
A program may use at most 256 MiB of HBM per device.

```python
import math
import jax
import jax.numpy as jnp
from jax import lax

EMBED_WIDTH = 2048
CHANNEL_COUNT = 64
ATTENDER_COUNT = 32
LR = 64
FE = 512
GROUPS = 4
TOP = 6
EXPERTS = 32
SEQ_DEV = 16
SEQS = 512
CAP = 6
N_EP = 32


def draw_picked_specialists(key, part):
    group_size = EXPERTS // GROUPS
    half_rows = (SEQ_DEV + 1) // 2

    def one_device(device):
        base = jax.random.fold_in(jax.random.fold_in(key, 17), device)
        subkeys = jax.random.split(base, 5)
        ranking = jax.random.permutation(subkeys[0], SEQ_DEV)
        first_group = jax.random.randint(subkeys[1], (), 0, GROUPS)
        other_group = (first_group + 1 + jax.random.randint(subkeys[2], (), 0, GROUPS - 1)) % GROUPS
        leading = ranking < half_rows
        group_ids = jnp.where(leading, first_group, other_group)
        within_group = jnp.where(leading, ranking, ranking - half_rows)
        order_first = jax.random.permutation(subkeys[3], group_size)
        order_other = jax.random.permutation(subkeys[4], group_size)
        positions = (within_group[:, None] * TOP + jnp.arange(TOP)[None, :]) % group_size
        chosen = jnp.where(leading[:, None], order_first[positions], order_other[positions])
        return (group_ids[:, None] * group_size + chosen).astype(jnp.int32)
    blocks = jax.vmap(one_device)(jnp.arange(N_EP))
    return blocks.reshape(SEQ_DEV * N_EP, TOP)


def steps_of(own_key, shape, shards, low, largest):
    level = 1.0
    for axis_at, blocks in shards:
        heights = jax.random.uniform(jax.random.fold_in(jax.random.fold_in(own_key, 6), axis_at), (blocks,), jnp.float32, low / len(shards), largest / len(shards))
        level = level * jnp.repeat(jnp.exp(heights), shape[axis_at] // blocks).reshape((-1,) + (1,) * (len(shape) - 1 - axis_at))
    return level


def bell_draw(own_key, shape, spread, reach, shards=(), kind=jnp.bfloat16):
    drawn = spread * jax.random.normal(own_key, shape, jnp.float32)
    if shards:
        drawn = drawn * steps_of(own_key, shape, shards, -0.22, 0.18)
    return jnp.clip(drawn, -reach, reach).astype(kind)


def setup_inputs(seed: int = 0) -> dict:
    arg_keys = jax.random.split(jax.random.key(seed), 24)
    latest_embeddings = bell_draw(arg_keys[0], (SEQS, EMBED_WIDTH), 1.0, 6.0, ((0, 32),))
    prior_memory_grids = bell_draw(arg_keys[1], (SEQS, ATTENDER_COUNT, CHANNEL_COUNT * CHANNEL_COUNT), 0.3, 1.75, ((0, 32),), jnp.float32)
    earlier_rescale_gain = jnp.clip(1.0 + 0.18 * jax.random.normal(arg_keys[2], (EMBED_WIDTH,), jnp.float32), 0.1, 1.9)
    query_map = bell_draw(arg_keys[3], (EMBED_WIDTH, EMBED_WIDTH), EMBED_WIDTH ** -0.5, 0.125, ((1, 32),))
    lookup_map = bell_draw(arg_keys[4], (EMBED_WIDTH, EMBED_WIDTH), EMBED_WIDTH ** -0.5, 0.125, ((1, 32),))
    content_map = bell_draw(arg_keys[5], (EMBED_WIDTH, EMBED_WIDTH), EMBED_WIDTH ** -0.5, 0.125, ((1, 32),))
    forget_lower_map = bell_draw(arg_keys[6], (EMBED_WIDTH, LR), EMBED_WIDTH ** -0.5, 0.125)
    forget_upper_map = bell_draw(arg_keys[7], (LR, EMBED_WIDTH), LR ** -0.5, 0.75)
    forget_shift = jnp.clip(jax.random.uniform(arg_keys[8], (EMBED_WIDTH,), jnp.float32, -3.0, 3.0), -3.0, 3.0)
    adapt_lower_map = bell_draw(arg_keys[9], (EMBED_WIDTH, LR), EMBED_WIDTH ** -0.5, 0.125)
    adapt_upper_map = bell_draw(arg_keys[10], (LR, EMBED_WIDTH), LR ** -0.5, 0.75)
    adapt_shift = jnp.clip(jax.random.uniform(arg_keys[11], (EMBED_WIDTH,), jnp.float32, -2.0, 2.0), -2.0, 2.0)
    erase_lookup_gains = jnp.clip(1.0 + 0.18 * jax.random.normal(arg_keys[12], (EMBED_WIDTH,), jnp.float32), 0.1, 1.9)
    substitute_lookup_gains = jnp.clip(1.0 + 0.18 * jax.random.normal(arg_keys[13], (EMBED_WIDTH,), jnp.float32), 0.1, 1.9)
    present_extra_gains = bell_draw(arg_keys[14], (EMBED_WIDTH,), 0.3, 1.75, (), jnp.float32)
    attender_rescale_gain = jnp.clip(1.0 + 0.18 * jax.random.normal(arg_keys[15], (EMBED_WIDTH,), jnp.float32), 0.1, 1.9)
    result_map = bell_draw(arg_keys[16], (EMBED_WIDTH, EMBED_WIDTH), EMBED_WIDTH ** -0.5, 0.125, ((1, 32),))
    later_rescale_gain = jnp.clip(1.0 + 0.18 * jax.random.normal(arg_keys[17], (EMBED_WIDTH,), jnp.float32), 0.1, 1.9)
    specialist_switch_maps = bell_draw(arg_keys[18], (EXPERTS, EMBED_WIDTH, FE), EMBED_WIDTH ** -0.5, 0.125, ((0, 32),))
    specialist_widen_maps = bell_draw(arg_keys[19], (EXPERTS, EMBED_WIDTH, FE), EMBED_WIDTH ** -0.5, 0.125, ((0, 32),))
    specialist_shrink_maps = bell_draw(arg_keys[20], (EXPERTS, FE, EMBED_WIDTH), FE ** -0.5, 0.25, ((0, 32),))
    picked_specialists = draw_picked_specialists(jax.random.fold_in(arg_keys[23], 71), 0)
    specialist_picked_shares = jnp.clip(jnp.exp(math.log(0.5) - 3.218876 * jax.random.uniform(arg_keys[22], (SEQS, TOP), jnp.float32) ** steps_of(arg_keys[22], (SEQS, TOP), ((0, 32),), -0.2, 0.2)), 0.02, 0.5)
    return dict(latest_embeddings=latest_embeddings, prior_memory_grids=prior_memory_grids, earlier_rescale_gain=earlier_rescale_gain, query_map=query_map, lookup_map=lookup_map, content_map=content_map, forget_lower_map=forget_lower_map, forget_upper_map=forget_upper_map, forget_shift=forget_shift, adapt_lower_map=adapt_lower_map, adapt_upper_map=adapt_upper_map, adapt_shift=adapt_shift, erase_lookup_gains=erase_lookup_gains, substitute_lookup_gains=substitute_lookup_gains, present_extra_gains=present_extra_gains, attender_rescale_gain=attender_rescale_gain, result_map=result_map, later_rescale_gain=later_rescale_gain, specialist_switch_maps=specialist_switch_maps, specialist_widen_maps=specialist_widen_maps, specialist_shrink_maps=specialist_shrink_maps, picked_specialists=picked_specialists, specialist_picked_shares=specialist_picked_shares)


norm_eps = 1e-06
group_eps = 0.00064
unit_eps = 1e-06

def rms_norm(rows_in, gain):
    values = rows_in.astype(jnp.float32)
    scale = lax.rsqrt(lax.optimization_barrier(jnp.mean(values * values, axis=-1, keepdims=True)) + norm_eps)
    return (values * scale * gain.astype(jnp.float32)).astype(jnp.bfloat16)

def memory_readout(query_signal, substitute_lookup, content_signals, forget_multiplier, adapt_speed, erase_signal, memory_grid, attender_rescale_gain, present_extra_gains):
    highest = lax.Precision.HIGHEST
    removed = jnp.einsum('bhij,bhj->bhi', memory_grid, erase_signal, precision=highest)
    memory_grid = memory_grid * forget_multiplier[:, :, None, :] - removed[..., None] * (erase_signal * adapt_speed)[:, :, None, :] + content_signals[..., None] * substitute_lookup[:, :, None, :]
    readout = jnp.einsum('bhij,bhj->bhi', memory_grid, query_signal, precision=highest)
    centered = readout - lax.optimization_barrier(jnp.mean(readout, axis=-1, keepdims=True))
    variance = lax.optimization_barrier(jnp.mean(centered * centered, axis=-1, keepdims=True))
    rescaled_result = centered * lax.rsqrt(variance + group_eps) * attender_rescale_gain
    present_extra = lax.optimization_barrier(jnp.sum(query_signal * substitute_lookup * present_extra_gains, axis=-1, keepdims=True)) * content_signals
    return (rescaled_result + present_extra, memory_grid)

def reference(latest_embeddings, prior_memory_grids, earlier_rescale_gain, query_map, lookup_map, content_map, forget_lower_map, forget_upper_map, forget_shift, adapt_lower_map, adapt_upper_map, adapt_shift, erase_lookup_gains, substitute_lookup_gains, present_extra_gains, attender_rescale_gain, result_map, later_rescale_gain, specialist_switch_maps, specialist_widen_maps, specialist_shrink_maps, picked_specialists, specialist_picked_shares):
    normed = rms_norm(latest_embeddings, earlier_rescale_gain)
    query_signal = jnp.dot(normed, query_map, preferred_element_type=jnp.float32).astype(jnp.bfloat16)
    key_rows = jnp.dot(normed, lookup_map, preferred_element_type=jnp.float32).astype(jnp.bfloat16)
    content_signals = jnp.dot(normed, content_map, preferred_element_type=jnp.float32).astype(jnp.bfloat16)
    decay_low = jnp.tanh(jnp.dot(normed, forget_lower_map, preferred_element_type=jnp.float32)).astype(jnp.bfloat16)
    forget_multiplier = jnp.exp(-math.exp(-0.5) * jax.nn.sigmoid(forget_shift + jnp.dot(decay_low, forget_upper_map, preferred_element_type=jnp.float32)))
    rate_low = jnp.dot(normed, adapt_lower_map, preferred_element_type=jnp.float32).astype(jnp.bfloat16)
    adapt_speed = jax.nn.sigmoid(adapt_shift + jnp.dot(rate_low, adapt_upper_map, preferred_element_type=jnp.float32))
    key_float = key_rows.astype(jnp.float32)
    erase_signal = (key_float * erase_lookup_gains).reshape(SEQS, ATTENDER_COUNT, CHANNEL_COUNT)
    erase_signal = erase_signal * lax.rsqrt(lax.optimization_barrier(jnp.sum(erase_signal * erase_signal, axis=-1, keepdims=True)) + unit_eps)
    substitute_lookup = key_float * (1.0 + (adapt_speed - 1.0) * substitute_lookup_gains)

    def blocked(array):
        return array.reshape(N_EP, SEQ_DEV, ATTENDER_COUNT, CHANNEL_COUNT)

    def one_block(block_entry_signal):
        return memory_readout(*block_entry_signal, attender_rescale_gain.reshape(ATTENDER_COUNT, CHANNEL_COUNT), present_extra_gains.reshape(ATTENDER_COUNT, CHANNEL_COUNT))
    mixed_parts, state_parts = lax.map(one_block, (blocked(query_signal.astype(jnp.float32)), blocked(substitute_lookup), blocked(content_signals.astype(jnp.float32)), blocked(forget_multiplier), blocked(adapt_speed), erase_signal.reshape(N_EP, SEQ_DEV, ATTENDER_COUNT, CHANNEL_COUNT), prior_memory_grids.reshape(N_EP, SEQ_DEV, ATTENDER_COUNT, CHANNEL_COUNT, CHANNEL_COUNT)))
    mixed = mixed_parts.reshape(SEQS, EMBED_WIDTH).astype(jnp.bfloat16)
    new_state = state_parts.reshape(SEQS, ATTENDER_COUNT, CHANNEL_COUNT * CHANNEL_COUNT)
    mixer_out = jnp.dot(mixed, result_map, preferred_element_type=jnp.float32).astype(jnp.bfloat16)
    residual = (latest_embeddings.astype(jnp.float32) + mixer_out.astype(jnp.float32)).astype(jnp.bfloat16)
    second = rms_norm(residual, later_rescale_gain)
    slot_count = N_EP * CAP
    flat_ids = picked_specialists.reshape(-1).astype(jnp.int32)

    def one_expert(block_entry_signal):
        expert_id, gate_w, up_w, down_w = block_entry_signal
        matched = flat_ids == expert_id
        ranking = jnp.argsort(jnp.where(matched, 0, 1).astype(jnp.int32), stable=True)[:slot_count].astype(jnp.int32)
        picked_rows = second[ranking // TOP]
        gate_proj = jnp.dot(picked_rows, gate_w, preferred_element_type=jnp.float32)
        up_proj = jnp.dot(picked_rows, up_w, preferred_element_type=jnp.float32)
        hidden_act = (jax.nn.silu(gate_proj) * up_proj).astype(jnp.bfloat16)
        results = jnp.dot(hidden_act, down_w, preferred_element_type=jnp.float32).astype(jnp.bfloat16)
        return (results, ranking, matched[ranking])
    outputs, rankings, is_valid = lax.map(one_expert, (jnp.arange(EXPERTS, dtype=jnp.int32), specialist_switch_maps, specialist_widen_maps, specialist_shrink_maps))
    coefficient = specialist_picked_shares.reshape(-1)[rankings] * is_valid.astype(specialist_picked_shares.dtype)
    contrib = (coefficient[..., None] * outputs.astype(specialist_picked_shares.dtype)).reshape(-1, EMBED_WIDTH)
    expert_sum = jnp.zeros((SEQS, EMBED_WIDTH), specialist_picked_shares.dtype).at[(rankings // TOP).reshape(-1)].add(contrib)
    new_hidden = (residual.astype(jnp.float32) + expert_sum).astype(jnp.bfloat16)
    return (new_hidden, new_state)
```

```python
import functools
import math

import jax
import jax.numpy as jnp
from jax import lax
from jax.experimental import pallas as pl
from jax.experimental.pallas import tpu as pltpu
from jax.sharding import PartitionSpec as P

GROUPS = 4
MESH = pl.DeviceIdType.MESH
HEAD_PAD = 8

norm_eps = 1e-06
group_eps = 0.00064
unit_eps = 1e-06

f32, bf16 = jnp.float32, jnp.bfloat16


def matmul_t(a, b):
    return lax.dot_general(a, b, (((1,), (1,)), ((), ())), preferred_element_type=f32)


def matmul(a, b):
    return jnp.dot(a, b, preferred_element_type=f32)


def iota(shape, axis):
    return lax.broadcasted_iota(jnp.int32, shape, axis)


def layer_kernel(
    devices,
    x_hbm, m_hbm, wq_hbm, wk_hbm, wv_hbm, wo_hbm, fl_hbm, fu_hbm, al_hbm, au_hbm,
    vec0, vec1, vec2, vec3, vec4, vec5, vec6, vec7,
    wg_hbm, wu_hbm, wd_hbm, pick_hbm, share_hbm,
    hid_ref, m_ref,
    tok, mix, wall, wo, low, vecs, picks, shares, wgb, wub, wdb,
    picker, spread, gains, rows_s, own_s, rem_s, result, landed, xcol, rescol,
    resland, rmsg, zsrc, disp, acc, sshare, part, pland, retsrc, rland,
    loc, psem_s, psem_r,
    az_s, az_r, au_s, au_r, aw_s, aw_r,
    bz_s, bz_r, bu_s, bu_r, bw_s, bw_r,
    cz_s, cz_r, cu_s, cu_r, cw_s, cw_r,
    ret_s, ret_r, msg_s, msg_r, res_s, res_r, sum_s, sum_r, home_s, home_r,
):
    me = lax.axis_index("ep")
    core, chip = me % 2, me // 2
    chips = devices // 2
    inner = chips // GROUPS
    side = math.isqrt(inner)
    layer, place = chip // inner, chip % inner
    along_y, along_x = place // side, place % side
    u = along_x * (1 - core) + along_y * core
    w = along_y * (1 - core) + along_x * core
    vp = w * side + u
    own = layer * inner + vp
    rows, depth = x_hbm.shape
    heads = m_hbm.shape[0] // rows
    span = depth // heads
    cells = m_hbm.shape[1]
    cw = depth // chips
    half = (rows + 1) // 2
    slots = inner * half
    group = devices // GROUPS
    pitch = heads + HEAD_PAD
    fe = wg_hbm.shape[2]

    def place_of(w_, u_):
        return (1 - core) * (w_ * side + u_) + core * (u_ * side + w_)

    def dev(l, w_, u_):
        return ((l * inner + place_of(w_, u_)) * 2 + core,)

    def lyr(j):
        return (layer + GROUPS - j) % GROUPS

    def rdma(src, dst, ss, rs, to):
        return pltpu.make_async_remote_copy(
            src_ref=src, dst_ref=dst, send_sem=ss, recv_sem=rs, device_id=to, device_id_type=MESH
        )

    partner = (me + 1 - 2 * core,)

    local = [(x_hbm, tok.at[own])]
    for i, ref in enumerate((wq_hbm, wk_hbm, wv_hbm)):
        local.append((ref, wall.at[i, core]))
    for i, ref in enumerate((fl_hbm, al_hbm, fu_hbm, au_hbm)):
        local.append((ref, low.at[i]))
    for i, ref in enumerate((vec0, vec1, vec2, vec3, vec4, vec5, vec6, vec7)):
        local.append((ref, vecs.at[pl.ds(i, 1)]))
    local += [(pick_hbm, picks), (share_hbm, shares), (wo_hbm, wo.at[core])]
    early = len(local)
    local.append((m_hbm, m_ref))
    for ref, buf in ((wg_hbm, wgb), (wu_hbm, wub), (wd_hbm, wdb)):
        local.append((ref.at[0], buf.at[core]))
    local = [pltpu.make_async_copy(s, d, loc.at[i]) for i, (s, d) in enumerate(local)]
    swaps = []
    for i, ref in enumerate((wq_hbm, wk_hbm, wv_hbm)):
        swaps.append((ref, wall.at[i, core]))
    swaps.append((wo_hbm, wo.at[core]))
    for ref, buf in ((wg_hbm, wgb), (wu_hbm, wub), (wd_hbm, wdb)):
        swaps.append((ref.at[0], buf.at[core]))
    swaps = [
        rdma(s, d, psem_s.at[i], psem_r.at[i], partner) for i, (s, d) in enumerate(swaps)
    ]

    for copy in local:
        copy.start()
    barrier = pltpu.get_barrier_semaphore()
    pl.semaphore_signal(barrier, inc=1, device_id=partner, device_id_type=MESH)

    def greet(k, carry):
        pl.semaphore_signal(
            barrier, inc=1, device_id=((me + 2 * k) % devices,), device_id_type=MESH
        )
        return carry

    lax.fori_loop(1, chips, greet, 0)

    def z_copy(buf, ss, rs, j):
        return rdma(buf.at[own], buf.at[own], ss.at[j], rs.at[j], dev((layer + j) % GROUPS, w, u))

    def u_copy(buf, ss, rs, j, r):
        block = buf.at[lyr(j) * inner + vp]
        return rdma(block, block, ss.at[j, r], rs.at[j, r], dev(layer, w, (u + r) % side))

    def w_copy(buf, ss, rs, j, r):
        block = buf.at[pl.ds(lyr(j) * inner + w * side, side)]
        return rdma(block, block, ss.at[j, r], rs.at[j, r], dev(layer, (w + r) % side, u))

    def u_start(buf, ss, rs, j):
        for r in range(1, side):
            u_copy(buf, ss, rs, j, r).start()

    def u_to_w(buf, us, ur, ws, wr, j):
        for r in range(1, side):
            u_copy(buf, us, ur, j, r).wait_recv()
        for r in range(1, side):
            w_copy(buf, ws, wr, j, r).start()

    def w_wait(buf, ws, wr, j):
        for r in range(1, side):
            w_copy(buf, ws, wr, j, r).wait_recv()

    def sends_done(buf, us, ur, ws, wr):
        for j in range(GROUPS):
            for r in range(1, side):
                u_copy(buf, us, ur, j, r).wait_send()
                w_copy(buf, ws, wr, j, r).wait_send()

    def spread_copy(src_of, dst, ss, rs, j, k):
        a, b = k // side, k % side
        l2, w2, u2 = lyr(j), (w + a) % side, (u + b) % side
        at = j * inner + k
        return rdma(src_of(l2, w2, u2), dst, ss.at[at], rs.at[at], dev(l2, w2, u2))

    def each(j, fn):
        def step(k, carry):
            fn(k)
            return carry

        lax.fori_loop(1 if j == 0 else 0, inner, step, 0)

    local[0].wait()
    pl.semaphore_wait(barrier, chips)
    for j in range(1, GROUPS):
        z_copy(tok, az_s, az_r, j).start()
    u_start(tok, au_s, au_r, 0)
    for i in range(4):
        swaps[i].start()
    for i in range(1, early):
        local[i].wait()

    lane = iota((1, 2 * span), 1)
    low_lane = lane < span

    shape = picker.shape
    picker[...] = jnp.where(iota(shape, 0) // span == iota(shape, 1) % span, 1.0, 0.0).astype(bf16)
    shape = spread.shape
    spread[...] = jnp.where(iota(shape, 1) // span == iota(shape, 0) % span, 1.0, 0.0).astype(bf16)

    def both_heads(tile):
        turned = pltpu.roll(tile, span, 1)
        return jnp.where(low_lane, tile, turned), jnp.where(low_lane, turned, tile)

    for i in range(4):
        for h in range(heads // 2):
            first, second = both_heads(vecs[3 + i : 4 + i, 2 * h * span : 2 * (h + 1) * span])
            gains[i, 2 * h : 2 * h + 1, :] = first
            gains[i, 2 * h + 1 : 2 * h + 2, :] = second

    def to_rows(slot, h, tile):
        first, second = both_heads(tile)
        rows_s[slot, pl.ds(2 * h, rows, stride=pitch), :] = first
        rows_s[slot, pl.ds(2 * h + 1, rows, stride=pitch), :] = second

    def normed_of(values, gain):
        values = values.astype(f32)
        scale = lax.rsqrt(jnp.mean(values * values, axis=-1, keepdims=True) + norm_eps)
        return (values * scale * gain).astype(bf16)

    mine = normed_of(tok[own], vecs[0:1, :])
    decay_low = jnp.tanh(matmul_t(mine, low[0])).astype(bf16)
    rate_low = matmul_t(mine, low[1]).astype(bf16)
    decay_all = vecs[1:2, :] + matmul(decay_low, low[2])
    rate_all = vecs[2:3, :] + matmul(rate_low, low[3])
    for h in range(heads // 2):
        part_at = slice(2 * h * span, 2 * (h + 1) * span)
        to_rows(3, h, decay_all[:, part_at])
        to_rows(4, h, rate_all[:, part_at])

    top = picks.shape[0]
    chosen = picks[...]
    weight = shares[...]
    eye = iota((rows, rows), 0) == iota((rows, rows), 1)
    before = iota((rows, rows), 0) < iota((rows, rows), 1)
    group_row = jnp.zeros((1, rows), f32)
    for g in range(1, GROUPS):
        group_row += jnp.where(chosen[0:1, :] >= g * group, 1.0, 0.0)

    def to_column(row):
        return jnp.sum(jnp.where(eye, jnp.broadcast_to(row, (rows, rows)), 0.0), axis=1, keepdims=True)

    group_col = to_column(group_row)
    rank_row = jnp.sum(
        jnp.where(jnp.logical_and(group_col == group_row, before), 1.0, 0.0), axis=0, keepdims=True
    )
    home_col = to_column(group_row * half + rank_row)
    per_tile = 128 // rows
    here = iota((1, 128), 1) // rows == vp % per_tile

    def placed(values):
        tiled = jnp.concatenate([values] * per_tile, axis=1)
        return jnp.where(here, tiled, 0.0)

    code = group_row * slots + (vp * half).astype(f32) + rank_row + 1.0
    local_ids = chosen.astype(f32) - group_row * group
    expert = iota((group, rows), 0).astype(f32)
    table = jnp.zeros((group, rows), f32)
    for t in range(top):
        table += jnp.where(expert == local_ids[t : t + 1, :], weight[t : t + 1, :], 0.0)
    rmsg[own, 0:8, :] = jnp.broadcast_to(placed(code), (8, 128))
    rmsg[own, 8 : 8 + group, :] = placed(table)

    per_step = min(inner, 4)

    def project_in(j):
        base = lyr(j) * inner

        def step(s, carry):
            at = base + s * per_step
            tokens = tok[pl.ds(at, per_step)].reshape(per_step * rows, depth)
            values = normed_of(tokens, vecs[0:1, :])
            product = matmul_t(values, wall[...].reshape(-1, depth)).astype(bf16)
            for c in range(per_step):
                result[at + c] = product[c * rows : (c + 1) * rows]
            start = pl.multiple_of(chip * cw // 128 * 128, 128)
            piece = tok[pl.ds(at, per_step), :, pl.ds(start, 128)].reshape(per_step * rows, 128)
            if cw < 128:
                piece = pltpu.roll(piece.astype(f32), (128 - chip * cw % 128) % 128, 1)
                piece = piece[:, :cw].astype(bf16)
            xcol[pl.ds(at, per_step)] = piece.reshape(per_step, rows, cw)
            return carry

        lax.fori_loop(0, inner // per_step, step, 0)
        each(j, lambda k: ret_copy(j, k).start())

    def ret_copy(j, k):
        return spread_copy(
            lambda l, a, b: result.at[l * inner + a * side + b], landed.at[chip], ret_s, ret_r, j, k
        )

    a_u, a_w = (tok, au_s, au_r), (tok, aw_s, aw_r)
    for j in range(1, GROUPS):
        z_copy(tok, az_s, az_r, j).wait_recv()
        u_start(*a_u, j)
        u_to_w(tok, au_s, au_r, aw_s, aw_r, j - 1)
    for i in range(3):
        swaps[i].wait()
    w_wait(*a_w, 0)
    project_in(0)
    u_to_w(tok, au_s, au_r, aw_s, aw_r, GROUPS - 1)
    landed[chip] = result[own]
    for j in range(1, GROUPS):
        w_wait(*a_w, j)
        project_in(j)
    for i in range(4, 7):
        swaps[i].start()

    def msg_copy(j, k):
        return spread_copy(lambda l, a, b: rmsg.at[own], rmsg.at[own], msg_s, msg_r, j, k)

    for j in range(GROUPS):
        each(j, lambda k: msg_copy(j, k).start())
    local[early].wait()
    for j in range(GROUPS):
        each(j, lambda k: ret_copy(j, k).wait_recv())

    pieces = max(1, 128 // cw)
    heads_of = 128 // (2 * span)
    for t in range(depth // 128):
        for i in range(3):
            tile = jnp.concatenate(
                [
                    landed[t * pieces + c][:, i * cw : i * cw + min(cw, 128)].astype(f32)
                    for c in range(pieces)
                ],
                axis=1,
            )
            to_rows(i, t * heads_of, tile)

    block = 2 * heads
    width = 4 * span
    chunks = cells // width

    def head_sum(v):
        return 0.5 * jnp.sum(v, axis=-1, keepdims=True)

    def wide(v):
        return jnp.concatenate([v, v], axis=1)

    def load_rows(ref, i):
        return jnp.concatenate(
            [ref[pl.ds(pl.multiple_of((2 * i + s) * pitch, 8), heads), :] for s in range(2)], axis=0
        )

    def gain(i):
        return jnp.concatenate([gains[i]] * 2, axis=0)

    def readout_step(i, carry):
        at = pl.multiple_of(i * block, block)
        q, k, v = (load_rows(rows_s.at[n], i) for n in range(3))
        decay = jnp.exp(-math.exp(-0.5) * jax.nn.sigmoid(load_rows(rows_s.at[3], i)))
        rate = jax.nn.sigmoid(load_rows(rows_s.at[4], i))
        erase = k * gain(0)
        erase = erase * lax.rsqrt(head_sum(erase * erase) + unit_eps)
        repl = k * (1.0 + (rate - 1.0) * gain(1))
        erase_rate = erase * rate
        erase_w, query_w = wide(erase), wide(decay * q)
        total = jnp.zeros((2 * block, 2 * span), f32)
        for c in range(chunks):
            cut = pl.ds(c * width, width)
            m = m_ref[pl.ds(at, block), cut]
            both = jnp.concatenate([(m * erase_w).astype(bf16), (m * query_w).astype(bf16)], axis=0)
            total += matmul(both, picker[cut, :])
        removed, kept = total[:block], total[block:]
        read = kept - removed * head_sum(erase_rate * q) + v * head_sum(repl * q)
        centered = read - head_sum(read) / span
        variance = head_sum(centered * centered) / span
        mixed = centered * lax.rsqrt(variance + group_eps) * gain(3)
        mixed = mixed + head_sum(q * repl * gain(2)) * v
        for s in range(2):
            cut = slice(s * heads, (s + 1) * heads)
            own_s[pl.ds(pl.multiple_of((2 * i + s) * pitch, 8), heads), :] = mixed[cut]
        rem_s[0, pl.ds(at, block), :] = removed
        rem_s[1, pl.ds(at, block), :] = decay
        rem_s[2, pl.ds(at, block), :] = erase_rate
        rem_s[3, pl.ds(at, block), :] = repl
        return carry

    lax.fori_loop(0, rows // 2, readout_step, 0)
    for h in range(heads // 2):
        first = own_s[pl.ds(2 * h, rows, stride=pitch), :]
        second = own_s[pl.ds(2 * h + 1, rows, stride=pitch), :]
        mix[own, :, 2 * h * span : 2 * (h + 1) * span] = jnp.where(low_lane, first, second).astype(
            bf16
        )

    def update_step(i, carry):
        at = pl.multiple_of(i * block, block)
        v = load_rows(rows_s.at[2], i)
        removed, decay, erase_rate, repl = (rem_s[n, pl.ds(at, block), :] for n in range(4))
        high = removed.astype(bf16).astype(f32)
        pair = jnp.where(low_lane, high, removed - high).astype(bf16)
        fresh = jnp.where(low_lane, v, 0.0).astype(bf16)
        stacked = jnp.concatenate([pair, fresh], axis=0)
        decay_w, rate_w, repl_w = wide(decay), wide(erase_rate), wide(repl)
        for c in range(chunks):
            cut = pl.ds(c * width, width)
            grown = matmul(stacked, spread[:, cut])
            m_ref[pl.ds(at, block), cut] = (
                m_ref[pl.ds(at, block), cut] * decay_w - grown[:block] * rate_w + grown[block:] * repl_w
            )
        return carry

    steps = rows // 2

    def update(start, stop):
        lax.fori_loop(start, stop, update_step, 0)

    b_u, b_w = (mix, bu_s, bu_r), (mix, bw_s, bw_r)
    for j in range(1, GROUPS):
        z_copy(mix, bz_s, bz_r, j).start()
    u_start(*b_u, 0)
    swaps[3].wait()
    for j in range(GROUPS):
        each(j, lambda k: msg_copy(j, k).wait_recv())
    update(0, steps // 4)
    for j in range(1, GROUPS):
        z_copy(mix, bz_s, bz_r, j).wait_recv()
        u_start(*b_u, j)
        u_to_w(mix, bu_s, bu_r, bw_s, bw_r, j - 1)
        update(j * steps // GROUPS, (j + 1) * steps // GROUPS)
    u_to_w(mix, bu_s, bu_r, bw_s, bw_r, GROUPS - 1)

    tiles = -(-inner // per_tile)

    def route_rows(sigma, row):
        parts = []
        for t in range(tiles):
            count = min(per_tile, inner - t * per_tile)
            total = rmsg[sigma * inner + t * per_tile, pl.ds(row, 1), :]
            for c in range(1, count):
                total += rmsg[sigma * inner + t * per_tile + c, pl.ds(row, 1), :]
            parts.append(total[:, : count * rows])
        return parts[0] if tiles == 1 else jnp.concatenate(parts, axis=1)

    def slot_copy(j, sigma):
        to = (layer + j) % GROUPS
        return rdma(
            zsrc.at[to, sigma], disp.at[own, sigma], cz_s.at[j, sigma], cz_r.at[j, sigma], dev(to, w, u)
        )

    def res_copy(j, k):
        return spread_copy(
            lambda l, a, b: rescol.at[l * inner + a * side + b], resland.at[chip], res_s, res_r, j, k
        )

    tokens_in = inner * rows
    first_expert = place * 2

    def project_out(j):
        sigma = lyr(j)
        base = sigma * inner
        tokens = mix[pl.ds(base, inner)].reshape(tokens_in, depth)
        product = matmul_t(tokens, wo[...].reshape(-1, depth)).astype(bf16)
        old = xcol[pl.ds(base, inner)].reshape(tokens_in, cw)
        res = (old.astype(f32) + product.astype(f32)).astype(bf16)
        for c in range(inner):
            rescol[base + c] = res[c * rows : (c + 1) * rows]
        codes = route_rows(sigma, 0)
        match = iota((GROUPS * slots, tokens_in), 0).astype(f32) + 1.0 == codes
        chosen_rows = matmul(jnp.where(match, 1.0, 0.0).astype(bf16), res).astype(bf16)
        for g in range(GROUPS):
            zsrc[g, sigma] = chosen_rows[g * slots : (g + 1) * slots]
        for g in range(1, GROUPS):
            slot_copy(g, sigma).start()
        disp[own, sigma] = zsrc[layer, sigma]
        ours = (
            iota((slots, tokens_in), 0).astype(f32) + (layer * slots).astype(f32) + 1.0 == codes
        )
        for e in range(2):
            held = route_rows(sigma, 8 + first_expert + e)
            sshare[e, pl.ds(pl.multiple_of(sigma * slots, slots), slots), :] = jnp.broadcast_to(
                jnp.sum(jnp.where(ours, held, 0.0), axis=1, keepdims=True), (slots, 128)
            )

    for j in range(GROUPS):
        w_wait(*b_w, j)
        project_out(j)
    for j in range(GROUPS):
        each(j, lambda k: res_copy(j, k).start())
    resland[chip] = rescol[own]

    every = GROUPS * slots
    c_u, c_w = (disp, cu_s, cu_r), (disp, cw_s, cw_r)

    def disp_u(j):
        if j:
            for s in range(GROUPS):
                slot_copy(j, s).wait_recv()
        u_start(*c_u, j)

    mblock = min(every, 128)

    def gate_up(j):
        d = lyr(j)
        k_at = pl.multiple_of(d * inner * cw, inner * cw)

        def step(i, carry):
            r_at = pl.multiple_of(i * mblock, mblock)
            parts = []
            for a in range(inner):
                ay, ax = a // side, a % side
                v = (1 - core) * a + core * (ax * side + ay)
                if every == mblock:
                    parts.append(disp[d * inner + v].reshape(every, cw))
                else:
                    parts.append(
                        disp[d * inner + v, r_at // slots, pl.ds(r_at % slots, mblock), :]
                    )
            cols = jnp.concatenate(parts, axis=1).astype(f32)
            squares = jnp.sum(cols * cols, axis=1, keepdims=True)
            cols = (cols * vecs[7:8, pl.ds(k_at, inner * cw)]).astype(bf16)
            at = pl.ds(r_at, mblock)
            squares = jnp.broadcast_to(squares, (mblock, 128))
            if j == 0:
                sshare[2, at, :] = squares
            else:
                sshare[2, at, :] += squares
            for e in range(2):
                for n, ref in enumerate((wgb, wub)):
                    cut = slice((2 * e + n) * fe, (2 * e + n + 1) * fe)
                    product = matmul(cols, ref[e, pl.ds(k_at, inner * cw), :])
                    if j == 0:
                        acc[at, cut] = product
                    else:
                        acc[at, cut] += product
            return carry

        lax.fori_loop(0, every // mblock, step, 0)

    disp_u(0)
    for j in range(1, GROUPS):
        disp_u(j)
        u_to_w(disp, cu_s, cu_r, cw_s, cw_r, j - 1)
    for i in range(early + 1, early + 4):
        local[i].wait()
    for i in range(4, 7):
        swaps[i].wait()
    w_wait(*c_w, 0)
    gate_up(0)
    u_to_w(disp, cu_s, cu_r, cw_s, cw_r, GROUPS - 1)
    for j in range(1, GROUPS):
        w_wait(*c_w, j)
        gate_up(j)

    def activate(i, carry):
        at = pl.ds(pl.multiple_of(i * mblock, mblock), mblock)
        scale = lax.rsqrt(sshare[2, at, 0:1] / depth + norm_eps)
        for e in range(2):
            gate = acc[at, 2 * e * fe : (2 * e + 1) * fe] * scale
            up = acc[at, (2 * e + 1) * fe : (2 * e + 2) * fe] * scale
            hidden = jax.nn.silu(gate) * up * sshare[e, at, 0:1]
            acc[at, e * fe : (e + 1) * fe] = hidden
        return carry

    lax.fori_loop(0, every // mblock, activate, 0)
    wide_cols = depth // 2
    step_cols = wide_cols // 2

    def sum_copy(n, k):
        a, b = k // side, k % side
        w2, u2 = (w + a) % side, (u + b) % side
        at = n * inner + k
        return rdma(
            part.at[n, w2 * side + u2], pland.at[n, k], sum_s.at[at], sum_r.at[at], dev(layer, w2, u2)
        )

    left = acc[:, 0:fe].astype(bf16)
    right = acc[:, fe : 2 * fe].astype(bf16)
    for n in range(2):
        for c in range(2):
            cut = slice(n * wide_cols + c * step_cols, n * wide_cols + (c + 1) * step_cols)
            total = matmul(left, wdb[0, :, cut]) + matmul(right, wdb[1, :, cut])
            for p in range(inner):
                piece = jnp.concatenate(
                    [
                        total[s * slots + p * half : s * slots + (p + 1) * half]
                        for s in range(GROUPS)
                    ],
                    axis=0,
                )
                part[n, p, :, c * step_cols : (c + 1) * step_cols] = piece.astype(bf16)
        for k in range(1, inner):
            sum_copy(n, k).start()

    sums = []
    for n in range(2):
        total = part[n, vp].astype(f32)
        for k in range(1, inner):
            sum_copy(n, k).wait_recv()
            total += pland[n, k].astype(f32)
        sums.append(total)
    for s in range(GROUPS):
        cut = slice(s * half, (s + 1) * half)
        retsrc[s] = jnp.concatenate([sums[0][cut], sums[1][cut]], axis=0).astype(bf16)

    def home_copy(j):
        to = (layer + j) % GROUPS
        return rdma(retsrc.at[to], rland.at[layer], home_s.at[j], home_r.at[j], dev(to, w, u))

    for j in range(1, GROUPS):
        home_copy(j).start()
    rland[layer] = retsrc[layer]
    for j in range(GROUPS):
        each(j, lambda k: res_copy(j, k).wait_recv())
    residual = jnp.concatenate([resland[c].astype(f32) for c in range(chips)], axis=1)
    find = home_col == iota((rows, GROUPS * half), 1).astype(f32)
    find = jnp.where(find, 1.0, 0.0).astype(bf16)
    for j in range(1, GROUPS):
        home_copy(j).wait_recv()
    back = [rland[g].astype(f32) for g in range(GROUPS)]
    for n in range(2):
        table = jnp.concatenate([b[n * half : (n + 1) * half] for b in back], axis=0).astype(bf16)
        cut = slice(n * wide_cols, (n + 1) * wide_cols)
        hid_ref[:, cut] = (residual[:, cut] + matmul(find, table)).astype(bf16)

    sends_done(tok, au_s, au_r, aw_s, aw_r)
    sends_done(mix, bu_s, bu_r, bw_s, bw_r)
    sends_done(disp, cu_s, cu_r, cw_s, cw_r)
    for j in range(1, GROUPS):
        z_copy(tok, az_s, az_r, j).wait_send()
        z_copy(mix, bz_s, bz_r, j).wait_send()
        home_copy(j).wait_send()
        for s in range(GROUPS):
            slot_copy(j, s).wait_send()
    for j in range(GROUPS):
        each(j, lambda k: ret_copy(j, k).wait_send())
        each(j, lambda k: msg_copy(j, k).wait_send())
        each(j, lambda k: res_copy(j, k).wait_send())
    for n in range(2):
        for k in range(1, inner):
            sum_copy(n, k).wait_send()


def local(
    latest_embeddings,
    prior_memory_grids,
    earlier_rescale_gain,
    query_map,
    lookup_map,
    content_map,
    forget_lower_map,
    forget_upper_map,
    forget_shift,
    adapt_lower_map,
    adapt_upper_map,
    adapt_shift,
    erase_lookup_gains,
    substitute_lookup_gains,
    present_extra_gains,
    attender_rescale_gain,
    result_map,
    later_rescale_gain,
    specialist_switch_maps,
    specialist_widen_maps,
    specialist_shrink_maps,
    picked_specialists,
    specialist_picked_shares,
):
    devices = lax.axis_size("ep")
    chips = devices // 2
    inner = chips // GROUPS
    side = math.isqrt(inner)
    rows, depth = latest_embeddings.shape
    _, heads, cells = prior_memory_grids.shape
    span = depth // heads
    columns = query_map.shape[1]
    cw = 2 * columns
    half = (rows + 1) // 2
    slots = inner * half
    every = GROUPS * slots
    group = devices // GROUPS
    fe = specialist_switch_maps.shape[2]
    rank = forget_lower_map.shape[1]
    padded = rows * (heads + HEAD_PAD)
    top = picked_specialists.shape[1]
    dma = pltpu.SemaphoreType.DMA
    vmem = pltpu.VMEM
    any_space = pl.BlockSpec(memory_space=pltpu.HBM)
    vector = [
        v.reshape(1, depth)
        for v in (
            earlier_rescale_gain,
            forget_shift,
            adapt_shift,
            erase_lookup_gains,
            substitute_lookup_gains,
            present_extra_gains,
            attender_rescale_gain,
            later_rescale_gain,
        )
    ]
    inputs = [
        latest_embeddings,
        prior_memory_grids.reshape(rows * heads, cells),
        query_map.T,
        lookup_map.T,
        content_map.T,
        result_map.T,
        forget_lower_map.T,
        forget_upper_map,
        adapt_lower_map.T,
        adapt_upper_map,
        *vector,
        specialist_switch_maps,
        specialist_widen_maps,
        specialist_shrink_maps,
        picked_specialists.T,
        specialist_picked_shares.T,
    ]
    relay_sems = [
        dma((GROUPS,)),
        dma((GROUPS,)),
        dma((GROUPS, side)),
        dma((GROUPS, side)),
        dma((GROUPS, side)),
        dma((GROUPS, side)),
    ]
    slot_sems = [dma((GROUPS, GROUPS)), dma((GROUPS, GROUPS))] + relay_sems[2:]
    hidden, state = pl.pallas_call(
        functools.partial(layer_kernel, devices),
        out_shape=[
            pltpu.VMEM((rows, depth), bf16),
            pltpu.VMEM((rows * heads, cells), f32),
        ],
        in_specs=[any_space] * len(inputs),
        out_specs=[pl.BlockSpec(memory_space=pltpu.VMEM)] * 2,
        scratch_shapes=[
            vmem((chips, rows, depth), bf16),
            vmem((chips, rows, depth), bf16),
            vmem((3, 2, columns, depth), bf16),
            vmem((2, columns, depth), bf16),
            vmem((4, rank, depth), bf16),
            vmem((8, depth), f32),
            vmem((top, rows), jnp.int32),
            vmem((top, rows), f32),
            vmem((2, depth, fe), bf16),
            vmem((2, depth, fe), bf16),
            vmem((2, fe, depth), bf16),
            vmem((cells, 2 * span), bf16),
            vmem((2 * span, cells), bf16),
            vmem((4, heads, 2 * span), f32),
            vmem((5, padded, 2 * span), f32),
            vmem((padded, 2 * span), f32),
            vmem((4, rows * heads, 2 * span), f32),
            vmem((chips, rows, 3 * cw), bf16),
            vmem((chips, rows, 3 * cw), bf16),
            vmem((chips, rows, cw), bf16),
            vmem((chips, rows, cw), bf16),
            vmem((chips, rows, cw), bf16),
            vmem((chips, 8 + group, 128), f32),
            vmem((GROUPS, GROUPS, slots, cw), bf16),
            vmem((chips, GROUPS, slots, cw), bf16),
            vmem((every, 4 * fe), f32),
            vmem((3, every, 128), f32),
            vmem((2, inner, GROUPS * half, depth // 2), bf16),
            vmem((2, inner, GROUPS * half, depth // 2), bf16),
            vmem((GROUPS, 2 * half, depth // 2), bf16),
            vmem((GROUPS, 2 * half, depth // 2), bf16),
            dma((24,)),
            dma((7,)),
            dma((7,)),
            *relay_sems,
            *relay_sems,
            *slot_sems,
            dma((chips,)),
            dma((chips,)),
            dma((chips,)),
            dma((chips,)),
            dma((chips,)),
            dma((chips,)),
            dma((2 * inner,)),
            dma((2 * inner,)),
            dma((GROUPS,)),
            dma((GROUPS,)),
        ],
        compiler_params=pltpu.CompilerParams(
            collective_id=0, has_side_effects=True, vmem_limit_bytes=55 * 2**20
        ),
        name="layer",
    )(*inputs)
    return hidden, state.reshape(prior_memory_grids.shape)


def solution(mesh):
    return jax.shard_map(
        local,
        mesh=mesh,
        in_specs=(
            P("ep", None),
            P("ep", None, None),
            P(),
            P(None, "ep"),
            P(None, "ep"),
            P(None, "ep"),
            P(),
            P(),
            P(),
            P(),
            P(),
            P(),
            P(),
            P(),
            P(),
            P(),
            P(None, "ep"),
            P(),
            P("ep", None, None),
            P("ep", None, None),
            P("ep", None, None),
            P("ep", None),
            P("ep", None),
        ),
        out_specs=(P("ep", None), P("ep", None, None)),
        check_vma=False,
    )
```
